32 devices in a mesh: rep: 4 (over z), fs: 4 (over y, x), tp: 2 (over core).
Axes of the slice: x: 2, y: 2, z: 4, core: 2. Of those that a mesh axis runs over, the one named last changes fastest.
Arguments:
- hidden_pre: bfloat16 [8192, 4096], P(('rep', 'fs'), 'tp'), may hold values from -6 to 6
- out_grad: bfloat16 [8192, 2048], P(('rep', 'fs')), may hold values from -8 to 8
- down_weight: bfloat16 [2048, 4096], P('fs', 'tp'), may hold values from -0.09375 to 0.09375
Outputs:
- hidden_grad: bfloat16 [8192, 4096], P(('rep', 'fs'), 'tp')
- weight_grad: float32 [2048, 4096], P('fs', 'tp')
The draws below stay inside these ranges and needn't reach their ends.
All inputs are finite; a program needn't handle non-finite values.
Results may differ from the reference program's by a relative error of at most 0.0049.
Values may be sent and summed in bfloat16 or wider, within the bound.
No kernel may reach another device: no remote copies, remote signals or barrier semaphores. Data moves between devices by JAX's collectives and lax.ppermute only.
A program may use at most 64 MiB of HBM per device.

```python
import jax
import jax.numpy as jnp
from jax import lax

D = 2048
FF = 4096
TOK_DEV = 512
TOKENS = 8192


def strengthened(array, key, source, target, shards_of, factor):
    def block_of(axis_at):
        return (jnp.arange(array.shape[axis_at]) // (array.shape[axis_at] // shards_of)).reshape((-1,) + (1,) * (array.ndim - 1 - axis_at))

    one_side = jax.random.permutation(key, shards_of)[block_of(target)]
    far = (block_of(target) + shards_of // 2) % shards_of
    return jnp.where((block_of(source) == one_side) | (block_of(source) == far), factor * array, array)


def level_of(key, dims, split, low, largest):
    def one(axis_at, parts):
        draws = jax.random.uniform(jax.random.fold_in(jax.random.fold_in(key, 6), axis_at), (parts,), jnp.float32, low / len(split), largest / len(split))
        return jnp.repeat(jnp.exp(draws), dims[axis_at] // parts).reshape((-1,) + (1,) * (len(dims) - axis_at - 1))

    level = one(*split[0])
    for cut in split[1:]:
        level = level * one(*cut)
    return level


def bell_draw(stream_key, shape, deviation, most, split=(), held_as=jnp.bfloat16):
    entries = deviation * jax.random.normal(stream_key, shape, jnp.float32)
    if split:
        entries = entries * level_of(stream_key, shape, split, -0.22, 0.18)
    return jnp.clip(entries, -most, most).astype(held_as)


def gaussian_with(key, dims, scale, limit, shards, heavy, held_as=jnp.bfloat16):
    result = scale * jax.random.normal(key, dims, jnp.float32)
    if shards:
        result = result * level_of(key, dims, shards, -0.22, 0.18)
    return jnp.clip(strengthened(result, jax.random.fold_in(key, 3), *heavy), -limit, limit).astype(held_as)


def setup_inputs(seed: int = 0) -> dict:
    key_list = jax.random.split(jax.random.key(seed), 4)
    hidden_pre = bell_draw(key_list[0], (TOKENS, FF), 1.0, 6.0, ((0, 16), (1, 2)))
    out_grad = gaussian_with(key_list[1], (TOKENS, D), 1.0, 8.0, ((0, 16),), (0, 1, 16, 2.0))
    down_weight = bell_draw(key_list[2], (D, FF), FF ** -0.5, 0.09375, ((0, 4), (1, 2)))
    return dict(hidden_pre=hidden_pre, out_grad=out_grad, down_weight=down_weight)


def reference(hidden_pre, out_grad, down_weight):
    count = TOKENS // TOK_DEV
    pre_blocks = hidden_pre.reshape(count, TOK_DEV, FF)
    grad_blocks = out_grad.reshape(count, TOK_DEV, D)

    def one_block(total, inputs):
        pre_rows, grad_rows = inputs
        positive = jnp.maximum(pre_rows.astype(jnp.float32), jnp.float32(0.0))
        back = jnp.dot(grad_rows, down_weight, preferred_element_type=jnp.float32)
        hidden_rows = (2.0 * positive * back).astype(jnp.bfloat16)
        act = (positive * positive).astype(jnp.bfloat16)
        part = lax.dot_general(grad_rows, act, (((0,), (0,)), ((), ())), preferred_element_type=jnp.float32)
        part = part.astype(jnp.bfloat16)
        return total + part.astype(jnp.float32), hidden_rows

    start = jnp.zeros((D, FF), jnp.float32)
    total, hidden_rows = lax.scan(one_block, start, (pre_blocks, grad_blocks))
    hidden_grad = hidden_rows.reshape(TOKENS, FF)
    weight_grad = total * jnp.float32(TOKENS ** -0.5)
    return hidden_grad, weight_grad
```

```python
import math

import jax
import jax.numpy as jnp
from jax import lax
from jax.experimental import pallas as pl
from jax.experimental.pallas import tpu as pltpu
from jax.sharding import PartitionSpec as P

COLUMN_CHUNKS = 2
SHARED_PARTS = 0


def swap(value, axis, mask):
    return lax.ppermute(value, axis, [(i, i ^ mask) for i in range(lax.axis_size(axis))])


def after(value, *others):
    return lax.optimization_barrier((value, *others))[0]


def place(position, mine, other, chunk, chunks, out):
    half, width = mine.shape
    blocks = position[1]
    piece = 2 * half // blocks

    def kernel(where, mine_ref, other_ref, *refs):
        k = pl.program_id(0) ^ where[0]
        row = pl.multiple_of((k % (blocks // 2)) * piece, piece)

        @pl.when(k < blocks // 2)
        def _():
            refs[-1][...] = mine_ref[pl.ds(row, piece), :].astype(jnp.float32)

        @pl.when(k >= blocks // 2)
        def _():
            refs[-1][...] = other_ref[pl.ds(row, piece), :].astype(jnp.float32)

    whole = pl.BlockSpec((half, width), lambda j, where: (0, 0))
    old = [] if out is None else [out]
    return pl.pallas_call(
        kernel,
        grid_spec=pltpu.PrefetchScalarGridSpec(
            num_scalar_prefetch=1,
            grid=(blocks,),
            in_specs=[whole, whole] + [pl.BlockSpec(memory_space=pl.ANY)] * len(old),
            out_specs=pl.BlockSpec((piece, width), lambda j, where: (j, chunk)),
        ),
        out_shape=jax.ShapeDtypeStruct((2 * half, width * chunks), jnp.float32),
        input_output_aliases={3: 0} if old else {},
        name=f"place{chunk}",
    )(position[0].reshape(1).astype(jnp.int32), mine, other, *old)


def body(hidden_pre, out_grad, down_weight):
    f32, bf16 = jnp.float32, jnp.bfloat16
    tokens, ff_local = hidden_pre.shape
    shard = down_weight.shape[0]
    groups, reps = lax.axis_size("fs"), lax.axis_size("rep")
    me, me_rep = lax.axis_index("fs"), lax.axis_index("rep")
    bits = [1 << i for i in range(groups.bit_length() - 1)]
    rep_bits = [1 << i for i in range(reps.bit_length() - 1)]
    orders = (bits, bits[::-1])
    scale = 1.0 / math.sqrt(tokens * reps * groups)
    near_first = sorted(range(groups), key=lambda k: (bin(k).count("1"), k))

    grads = [
        lax.dynamic_slice_in_dim(out_grad, (me ^ k) * shard, shard, axis=1) for k in range(groups)
    ]

    def halves_of(value):
        left = value.shape[1] // 2
        return [value[:, :left], value[:, left:]]

    def near(value):
        have = {0: halves_of(value)}
        have.update({k: [None, None] for k in bits})
        for turn in range(2):
            for k in bits:
                h = turn if k == 1 else 1 - turn
                have[k][h] = swap(have[0][h], "fs", k)
        return have

    def spread(have):
        for k in near_first:
            if k not in have:
                last = [max(b for b in bits if b & k), min(b for b in bits if b & k)]
                have[k] = [swap(have[k ^ last[h]][h], "fs", last[h]) for h in range(2)]
        return have

    shared = ff_local * SHARED_PARTS // 8
    low = shard // 2
    side = me_rep & 1
    if shared:
        early = near(lax.dynamic_slice(down_weight, (side * low, 0), (low, shared)))

    def part(k, columns):
        return lax.dot_general(
            grads[k], columns, (((0,), (0,)), ((), ())), preferred_element_type=f32
        )

    def act_of(columns):
        positive = jnp.maximum(columns.astype(f32), 0.0)
        return (positive * positive).astype(bf16)

    width = ff_local // (2 * COLUMN_CHUNKS)
    sums = []
    first_sends, second_sends, all_sends = [], [], []
    for c in range(COLUMN_CHUNKS):
        acts = []
        for h in range(2):
            start = (2 * c + h) * width
            columns = hidden_pre[:, start : start + width]
            acts.append(act_of(after(columns, *first_sends) if first_sends else columns))
        held = [None, None]
        first_sends, previous, second_sends = [], second_sends, []
        for step in range(len(bits)):
            sent = [
                sorted(
                    (k for k in (held[h] or range(groups)) if k & orders[h][step]),
                    key=lambda k: (-bin(k).count("1"), k),
                )
                for h in range(2)
            ]
            nxt = [{}, {}]
            for i in range(len(sent[0])):
                for h in range(2):
                    k, b = sent[h][i], orders[h][step]
                    if step == 0:
                        columns = acts[h]
                        if i and previous:
                            columns = after(columns, *previous)
                        value = part(k, columns).astype(bf16)
                        first_sends.append(value)
                    else:
                        value = held[h][k].astype(bf16)
                        second_sends.append(value)
                    nxt[h][k ^ b] = swap(value, "fs", b)
            for h in range(2):
                for k in nxt[h]:
                    mine = part(k, acts[h]) if step == 0 else held[h][k]
                    nxt[h][k] = mine + nxt[h][k].astype(f32)
            held = nxt
        all_sends += second_sends
        sums.append(jnp.concatenate([held[0][0], held[1][0]], axis=1))
        all_sends += first_sends
    if shared:
        for k in bits:
            early[k] = list(lax.optimization_barrier((*early[k], sums[0]))[:2])
        early = spread(early)
        other = {k: [swap(v, "rep", 1) for v in early[k]] for k in near_first[1:]}

    late = near(after(down_weight[:, shared:], sums[0], *all_sends))
    onward = [late[k][0 if k == 1 else 1] for k in bits]
    late = spread(late)

    position = sum(((me_rep >> i) & 1) * (reps >> (i + 1)) for i in range(len(rep_bits)))
    weight_grad = None
    for c, local in enumerate(sums):
        for i, b in enumerate(rep_bits):
            rows = local.shape[0] // 2
            bit = (me_rep >> i) & 1
            got = swap(
                lax.dynamic_slice_in_dim(local, (1 - bit) * rows, rows, 0).astype(bf16), "rep", b
            )
            local = lax.dynamic_slice_in_dim(local, bit * rows, rows, 0) + got.astype(f32)
        mine = (local * scale).astype(bf16)
        if c == COLUMN_CHUNKS - 1:
            mine = after(mine, *onward)
        for b in rep_bits[::-1]:
            theirs = swap(mine, "rep", b)
            if b != 1:
                mine = jnp.concatenate([mine, theirs], axis=0)
        weight_grad = place((position, reps), mine, theirs, c, COLUMN_CHUNKS, weight_grad)

    def finish(columns, blocks):
        back = None
        for g, w in blocks:
            term = jnp.dot(g, w, preferred_element_type=f32)
            back = term if back is None else back + term
        positive = jnp.maximum(hidden_pre[:, columns].astype(f32), 0.0)
        return (2.0 * positive * back).astype(bf16)

    hidden = []
    if shared:
        own = [lax.dynamic_slice_in_dim(g, side * low, low, axis=1) for g in grads]
        far = [lax.dynamic_slice_in_dim(g, (1 - side) * low, low, axis=1) for g in grads]
        for h in range(2):
            columns = slice(h * shared // 2, (h + 1) * shared // 2)
            blocks = [(grads[0], down_weight[:, columns])]
            for k in near_first[1:]:
                blocks += [(own[k], early[k][h]), (far[k], other[k][h])]
            hidden.append(finish(columns, blocks))
    middle = (ff_local - shared) // 2
    for h in range(2):
        columns = slice(shared + h * middle, shared + (h + 1) * middle)
        hidden.append(finish(columns, [(grads[k], late[k][h]) for k in near_first]))
    return jnp.concatenate(hidden, axis=1), weight_grad


def solution(mesh):
    placed = (P(("rep", "fs"), "tp"), P(("rep", "fs"), None), P("fs", "tp"))
    return jax.shard_map(
        body,
        mesh=mesh,
        in_specs=placed,
        out_specs=(P(("rep", "fs"), "tp"), P("fs", "tp")),
        check_vma=False,
    )
```

```python
import math

import jax
import jax.numpy as jnp
from jax import lax
from jax.experimental import pallas as pl
from jax.experimental.pallas import tpu as pltpu
from jax.sharding import PartitionSpec as P

COLUMN_CHUNKS = 2


def swap(value, axis, mask):
    return lax.ppermute(value, axis, [(i, i ^ mask) for i in range(lax.axis_size(axis))])


def after(value, *others):
    return lax.optimization_barrier((value, *others))[0]


def place(position, mine, other, chunk, chunks, out):
    half, width = mine.shape
    blocks = position[1]
    piece = 2 * half // blocks

    def kernel(where, mine_ref, other_ref, *refs):
        k = pl.program_id(0) ^ where[0]
        row = pl.multiple_of((k % (blocks // 2)) * piece, piece)

        @pl.when(k < blocks // 2)
        def _():
            refs[-1][...] = mine_ref[pl.ds(row, piece), :].astype(jnp.float32)

        @pl.when(k >= blocks // 2)
        def _():
            refs[-1][...] = other_ref[pl.ds(row, piece), :].astype(jnp.float32)

    whole = pl.BlockSpec((half, width), lambda j, where: (0, 0))
    old = [] if out is None else [out]
    return pl.pallas_call(
        kernel,
        grid_spec=pltpu.PrefetchScalarGridSpec(
            num_scalar_prefetch=1,
            grid=(blocks,),
            in_specs=[whole, whole] + [pl.BlockSpec(memory_space=pl.ANY)] * len(old),
            out_specs=pl.BlockSpec((piece, width), lambda j, where: (j, chunk)),
        ),
        out_shape=jax.ShapeDtypeStruct((2 * half, width * chunks), jnp.float32),
        input_output_aliases={3: 0} if old else {},
        name=f"place{chunk}",
    )(position[0].reshape(1).astype(jnp.int32), mine, other, *old)


def body(hidden_pre, out_grad, down_weight):
    f32, bf16 = jnp.float32, jnp.bfloat16
    tokens, ff_local = hidden_pre.shape
    shard = down_weight.shape[0]
    groups, reps = lax.axis_size("fs"), lax.axis_size("rep")
    me, me_rep = lax.axis_index("fs"), lax.axis_index("rep")
    bits = [1 << i for i in range(groups.bit_length() - 1)]
    rep_bits = [1 << i for i in range(reps.bit_length() - 1)]
    orders = (bits, bits[::-1])
    scale = 1.0 / math.sqrt(tokens * reps * groups)
    near_first = sorted(range(groups), key=lambda k: (bin(k).count("1"), k))

    grads = [
        lax.dynamic_slice_in_dim(out_grad, (me ^ k) * shard, shard, axis=1) for k in range(groups)
    ]

    def halves_of(value):
        left = value.shape[1] // 2
        return [value[:, :left], value[:, left:]]

    def near(value, gate):
        have = {0: halves_of(value)}
        have.update({k: [None, None] for k in bits})
        for turn in range(2):
            for k in bits:
                h = turn if k == 1 else 1 - turn
                part_sent = have[0][h]
                if turn and k != 1:
                    part_sent, gate = lax.optimization_barrier((part_sent, gate))
                have[k][h] = swap(part_sent, "fs", k)
        return have, gate

    def spread(have):
        for k in near_first:
            if k not in have:
                last = [max(b for b in bits if b & k), min(b for b in bits if b & k)]
                have[k] = [swap(have[k ^ last[h]][h], "fs", last[h]) for h in range(2)]
        return have

    def part(k, columns):
        return lax.dot_general(
            grads[k], columns, (((0,), (0,)), ((), ())), preferred_element_type=f32
        )

    def act_of(columns):
        positive = jnp.maximum(columns.astype(f32), 0.0)
        return (positive * positive).astype(bf16)

    width = ff_local // (2 * COLUMN_CHUNKS)
    sums = []
    first_sends, second_sends, all_sends = [], [], []
    for c in range(COLUMN_CHUNKS):
        acts = []
        for h in range(2):
            start = (2 * c + h) * width
            columns = hidden_pre[:, start : start + width]
            acts.append(act_of(after(columns, *first_sends) if first_sends else columns))
        held = [None, None]
        first_sends, previous, second_sends = [], second_sends, []
        for step in range(len(bits)):
            sent = [
                sorted(
                    (k for k in (held[h] or range(groups)) if k & orders[h][step]),
                    key=lambda k: (-bin(k).count("1"), k),
                )
                for h in range(2)
            ]
            nxt = [{}, {}]
            for i in range(len(sent[0])):
                for h in range(2):
                    k, b = sent[h][i], orders[h][step]
                    if step == 0:
                        columns = acts[h]
                        if i and previous:
                            columns = after(columns, *previous)
                        value = part(k, columns).astype(bf16)
                        first_sends.append(value)
                    else:
                        value = held[h][k].astype(bf16)
                        second_sends.append(value)
                    nxt[h][k ^ b] = swap(value, "fs", b)
            for h in range(2):
                for k in nxt[h]:
                    mine = part(k, acts[h]) if step == 0 else held[h][k]
                    nxt[h][k] = mine + nxt[h][k].astype(f32)
            held = nxt
        all_sends += second_sends
        sums.append(jnp.concatenate([held[0][0], held[1][0]], axis=1))
        all_sends += first_sends
    late, sums[0] = near(after(down_weight, sums[0], *all_sends), sums[0])
    onward = [late[k][0 if k == 1 else 1] for k in bits]
    late = spread(late)

    position = sum(((me_rep >> i) & 1) * (reps >> (i + 1)) for i in range(len(rep_bits)))
    ready = []
    for c, local in enumerate(sums):
        for i, b in enumerate(rep_bits):
            rows = local.shape[0] // 2
            bit = (me_rep >> i) & 1
            got = swap(
                lax.dynamic_slice_in_dim(local, (1 - bit) * rows, rows, 0).astype(bf16), "rep", b
            )
            local = lax.dynamic_slice_in_dim(local, bit * rows, rows, 0) + got.astype(f32)
        mine = (local * scale).astype(bf16)
        if c == COLUMN_CHUNKS - 1:
            mine = after(mine, *onward)
        for b in rep_bits[::-1]:
            theirs = swap(mine, "rep", b)
            if b != 1:
                mine = jnp.concatenate([mine, theirs], axis=0)
        ready.append((mine, theirs))

    def finish(columns, blocks):
        back = None
        for g, w in blocks:
            term = jnp.dot(g, w, preferred_element_type=f32)
            back = term if back is None else back + term
        positive = jnp.maximum(hidden_pre[:, columns].astype(f32), 0.0)
        return (2.0 * positive * back).astype(bf16)

    hidden = []
    middle = ff_local // 2
    for h in range(2):
        columns = slice(h * middle, (h + 1) * middle)
        hidden.append(finish(columns, [(grads[k], late[k][h]) for k in near_first]))
    hidden = jnp.concatenate(hidden, axis=1)
    weight_grad = None
    for c, (mine, theirs) in enumerate(ready):
        if c == COLUMN_CHUNKS - 1:
            theirs, hidden = lax.optimization_barrier((theirs, hidden))
        weight_grad = place((position, reps), mine, theirs, c, COLUMN_CHUNKS, weight_grad)
    return hidden, weight_grad


def solution(mesh):
    placed = (P(("rep", "fs"), "tp"), P(("rep", "fs"), None), P("fs", "tp"))
    return jax.shard_map(
        body,
        mesh=mesh,
        in_specs=placed,
        out_specs=(P(("rep", "fs"), "tp"), P("fs", "tp")),
        check_vma=False,
    )
```
